128 devices in a mesh: ep: 128 (over z, y, x, core).
Axes of the slice: x: 4, y: 4, z: 4, core: 2. Of those that a mesh axis runs over, the one named last changes fastest.
Arguments:
- tokens: bfloat16 [512, 2048], P('ep'), may hold values from -6 to 6
- lengths: int32 [512], P('ep'), may hold values from 1 to 1023
- cache_keys: bfloat16 [512, 1024, 2, 128], P('ep')
- cache_values: bfloat16 [512, 1024, 2, 128], P('ep'), may hold values from -6 to 6
- query_w: bfloat16 [2048, 1024], replicated, may hold values from -0.125 to 0.125
- key_w: bfloat16 [2048, 256], replicated, may hold values from -0.125 to 0.125
- value_w: bfloat16 [2048, 256], replicated, may hold values from -0.125 to 0.125
- out_w: bfloat16 [1024, 2048], replicated, may hold values from -0.1875 to 0.1875
- mix_lambda: float32 [8], replicated, may hold values from 0.3 to 0.8
- head_gain: float32 [128], replicated, may hold values from 0.1 to 1.9
- attn_gain: float32 [2048], replicated, may hold values from 0.1 to 1.9
- ffn_gain: float32 [2048], replicated, may hold values from 0.1 to 1.9
- routes: int32 [512, 2], P('ep'), may hold values from 0 to 7, all different within a row; in each aligned block of 4 rows (0 to 3, 4 to 7, ...) at most 2 rows name the same one
- route_weights: float32 [512, 2], P('ep'), may hold values from 0.2 to 1
- exp_gate: bfloat16 [2048, 49152], P(None, 'ep'), may hold values from -0.125 to 0.125
- exp_up: bfloat16 [2048, 49152], P(None, 'ep'), may hold values from -0.125 to 0.125
- exp_down: bfloat16 [49152, 2048], P('ep'), may hold values from -0.078125 to 0.078125
- dense_gate: bfloat16 [128, 256, 352], P('ep'), may hold values from -0.125 to 0.125
- dense_up: bfloat16 [128, 256, 352], P('ep'), may hold values from -0.125 to 0.125
- dense_down: bfloat16 [128, 352, 256], P('ep'), may hold values from -0.078125 to 0.078125
- branch_gate: bfloat16 [2048], replicated, may hold values from -0.125 to 0.125
Outputs:
- output: bfloat16 [512, 2048], P('ep')
- new_keys: bfloat16 [512, 256], P('ep')
- new_values: bfloat16 [512, 256], P('ep')
The draws below stay inside these ranges and needn't reach their ends.
Inputs may be any that keep to these rules, and one draw needn't show every extreme that they name: `routes`: each row names 2 different experts; among the 4 rows of one device no expert is named by more than 2 rows, a bound that some block reaches.
All inputs are finite; a program needn't handle non-finite values.
Results may differ from the reference program's by a relative error of at most 0.015.
Values may be sent and summed in bfloat16 or wider, within the bound.
A program may use at most 128 MiB of HBM per device.

```python
import math
import jax
import jax.numpy as jnp
import numpy as np
from jax import lax

D = 2048
HEADS = 8
KV_HEADS = 2
HEAD_DIM = 128
CACHE = 1024
SEQ_DEV = 4
TOP_K = 2
SPLIT = 16
EXP_FF = 6144
DENSE_FF = 5632
EXPERTS = 8
BLOCKS = 8
CAP = 2
TOKENS = 512
N_EP = 128


def draw_cache_keys(key, part):
    shape = (TOKENS, CACHE, KV_HEADS, HEAD_DIM)
    base_key = jax.random.fold_in(jax.random.fold_in(key, 11), 0)
    values = jax.random.normal(base_key, shape, jnp.float32) * 1.75
    values = jnp.clip(values, -10.0, 10.0)
    return values.astype(jnp.bfloat16)


def plant(drawn, stream_key, least, high):
    longest = drawn.shape.index(max(drawn.shape))
    spots = []
    for shift in (0, 1):
        where = [jax.random.randint(jax.random.fold_in(stream_key, axis), (), 0, length) for axis, length in enumerate(drawn.shape)]
        where[longest] = (where[longest] + shift) % drawn.shape[longest]
        spots.append(tuple(where))
    return drawn.at[spots[0]].set(least).at[spots[1]].set(high)


def level_of(key, extent, cuts, low, top_value):
    level = 1.0
    for position, blocks in cuts:
        steps = jax.random.uniform(jax.random.fold_in(jax.random.fold_in(key, 6), position), (blocks,), jnp.float32, low / len(cuts), top_value / len(cuts))
        level = level * jnp.repeat(jnp.exp(steps), extent[position] // blocks).reshape((-1,) + (1,) * (len(extent) - 1 - position))
    return level


def deal_out(own_key, own, number, rows, number_of, top, most, lean):
    ranking = jax.random.permutation(own_key, number_of)
    packed, ordinary = load_shares(number_of, rows * top, most, lean, True), load_shares(number_of, rows * top, most, lean, False)
    places = jnp.arange(number_of)

    def named(sizes, offset_by):
        used = int((sizes > 0).sum())
        fixed = max(1, used // 4)
        passed = fixed + (places - fixed + offset_by * (used - fixed)) % max(1, number_of - fixed)
        return jnp.zeros((number_of,), jnp.int32).at[ranking[jnp.where(places < fixed, places, passed)]].set(jnp.asarray(sizes, jnp.int32))

    sizes = jnp.where(number % 4 == 0, named(packed, number // 4), named(ordinary, number - number // 4 - 1))
    mixed = jax.random.permutation(jax.random.fold_in(own, 3), number_of)
    source_of, receiver = mixed[0:number_of // 2 * 2:2], mixed[1:number_of // 2 * 2:2]
    slack = jnp.minimum(sizes[source_of] - 1, most - sizes[receiver]) // 2
    slack = jnp.where((source_of == ranking[0]) | (receiver == ranking[0]) | (sizes[receiver] == 0), 0, jnp.maximum(slack, 0))
    passed = jax.random.randint(jax.random.fold_in(own, 4), (number_of // 2,), 0, 1 << 20) % (slack + 1)
    sizes = sizes.at[source_of].add(-passed).at[receiver].add(passed)
    members = jnp.searchsorted(jnp.cumsum(sizes), jnp.arange(rows * top), side="right").astype(jnp.int32)
    listing = members.reshape(top, rows).T
    listing = listing[jax.random.permutation(jax.random.fold_in(own, 1), rows)]
    offset_by = jax.random.randint(jax.random.fold_in(own, 2), (rows, 1), 0, top)
    return jnp.take_along_axis(listing, (jnp.arange(top)[None, :] + offset_by) % top, axis=1)


def load_shares(count, total, limit, skew, full):
    loads = [(1 << 20) // math.isqrt(grade ** skew) + 1 for grade in range(1, count + 1)]
    largest = limit if full else min(limit, max(-(-total // count), total * loads[0] // sum(loads)))
    least = 1 if total - largest >= count - 1 else 0
    counts, spare = [largest] + [least] * (count - 1), total - largest - least * (count - 1)
    while spare > 0:
        free = [i for i in range(1, count) if counts[i] < largest] or [i for i in range(1, count) if counts[i] < limit]
        mass, left = sum([loads[i] for i in free]), spare
        for i in free:
            extra = min(limit - counts[i], max(1, left * loads[i] // mass), spare)
            counts[i] = counts[i] + extra
            spare = spare - extra
    return np.array(counts)


def centred(key, extent, spread, most, shards=(), kind=jnp.bfloat16):
    values = jax.random.normal(key, extent, jnp.float32) * spread
    if len(shards) > 0:
        values = level_of(key, extent, shards, -0.22, 0.18) * values
    return jnp.clip(values, min=-most, max=most).astype(kind)


def setup_inputs(seed: int = 0) -> dict:
    seeds = jax.random.split(jax.random.key(seed), 22)
    tokens = centred(seeds[0], (TOKENS, D), 1.0, 6.0, ((0, 128),))
    lengths = plant(jax.random.randint(seeds[1], (TOKENS,), 1, CACHE), jax.random.fold_in(seeds[1], 1), 1, CACHE - 1).astype(jnp.int32)
    cache_keys = draw_cache_keys(jax.random.fold_in(seeds[21], 71), 0)
    cache_values = centred(seeds[3], (TOKENS, CACHE, KV_HEADS, HEAD_DIM), 1.0, 6.0, ((0, 128),))
    query_w = centred(seeds[4], (D, HEADS * HEAD_DIM), D ** -0.5, 0.125)
    key_w = centred(seeds[5], (D, KV_HEADS * HEAD_DIM), D ** -0.5, 0.125)
    value_w = centred(seeds[6], (D, KV_HEADS * HEAD_DIM), D ** -0.5, 0.125)
    out_w = centred(seeds[7], (HEADS * HEAD_DIM, D), (HEADS * HEAD_DIM) ** -0.5, 0.1875)
    mix_lambda = jnp.clip(jax.random.uniform(seeds[8], (HEADS,), jnp.float32, 0.3, 0.8), 0.3, 0.8)
    head_gain = jnp.clip(1.0 + 0.18 * jax.random.normal(seeds[9], (HEAD_DIM,), jnp.float32), 0.1, 1.9)
    attn_gain = jnp.clip(1.0 + 0.18 * jax.random.normal(seeds[10], (D,), jnp.float32), 0.1, 1.9)
    ffn_gain = jnp.clip(1.0 + 0.18 * jax.random.normal(seeds[11], (D,), jnp.float32), 0.1, 1.9)
    routes_keys = jax.random.split(jax.random.fold_in(seeds[12], 1), TOKENS // SEQ_DEV)
    routes_turns = jax.random.permutation(jax.random.fold_in(seeds[12], 3), TOKENS // SEQ_DEV)
    routes = jax.vmap(lambda own, number: deal_out(jax.random.fold_in(seeds[12], 2), own, number, SEQ_DEV, EXPERTS, TOP_K, CAP, 1))(routes_keys, routes_turns).reshape((TOKENS, TOP_K))
    route_weights = jnp.clip(0.2 + 0.8 * jax.random.uniform(seeds[13], (TOKENS, TOP_K), jnp.float32) ** level_of(seeds[13], (TOKENS, TOP_K), ((0, 128),), -0.2, 0.2), 0.2, 1.0)
    exp_gate = centred(seeds[14], (D, EXPERTS * EXP_FF), D ** -0.5, 0.125, ((1, 128),))
    exp_up = centred(seeds[15], (D, EXPERTS * EXP_FF), D ** -0.5, 0.125, ((1, 128),))
    exp_down = centred(seeds[16], (EXPERTS * EXP_FF, D), EXP_FF ** -0.5, 0.078125, ((0, 128),))
    dense_gate = centred(seeds[17], (N_EP, D // BLOCKS, DENSE_FF // SPLIT), D ** -0.5, 0.125, ((0, 128),))
    dense_up = centred(seeds[18], (N_EP, D // BLOCKS, DENSE_FF // SPLIT), D ** -0.5, 0.125, ((0, 128),))
    dense_down = centred(seeds[19], (N_EP, DENSE_FF // SPLIT, D // BLOCKS), DENSE_FF ** -0.5, 0.078125, ((0, 128),))
    branch_gate = centred(seeds[20], (D,), D ** -0.5, 0.125)
    return {"tokens": tokens, "lengths": lengths, "cache_keys": cache_keys, "cache_values": cache_values, "query_w": query_w, "key_w": key_w, "value_w": value_w, "out_w": out_w, "mix_lambda": mix_lambda, "head_gain": head_gain, "attn_gain": attn_gain, "ffn_gain": ffn_gain, "routes": routes, "route_weights": route_weights, "exp_gate": exp_gate, "exp_up": exp_up, "exp_down": exp_down, "dense_gate": dense_gate, "dense_up": dense_up, "dense_down": dense_down, "branch_gate": branch_gate}


def rms_norm(values, gain, epsilon):
    scale = lax.rsqrt(lax.optimization_barrier(jnp.mean(values * values, axis=-1, keepdims=True)) + epsilon)
    return values * scale * gain.astype(jnp.float32)

def softmax_pair(scores, own_score, valid):
    masked = jnp.where(valid, scores, -jnp.inf)
    largest = jnp.maximum(lax.optimization_barrier(jnp.max(masked, axis=-1)), own_score)
    raised = jnp.where(valid, jnp.exp(scores - largest[..., None]), 0.0)
    own_raised = jnp.exp(own_score - largest)
    total = lax.optimization_barrier(jnp.sum(raised, axis=-1)) + own_raised
    return (raised / total[..., None], own_raised / total)

def attend_block(tokens, lengths, cache_keys, cache_values, query_w, key_w, value_w, out_w, mix_lambda, head_gain, attn_gain, ffn_gain):
    rows = tokens.shape[0]
    groups = HEADS // KV_HEADS
    half = HEAD_DIM // 2
    scale = (HEAD_DIM // 2) ** (-0.5)
    xfull = tokens.astype(jnp.float32)
    normed = rms_norm(xfull, attn_gain, 1e-06).astype(jnp.bfloat16)
    query = jnp.dot(normed, query_w, preferred_element_type=jnp.float32).astype(jnp.bfloat16)
    key_new = jnp.dot(normed, key_w, preferred_element_type=jnp.float32).astype(jnp.bfloat16)
    value_new = jnp.dot(normed, value_w, preferred_element_type=jnp.float32).astype(jnp.bfloat16)
    qfull = query.astype(jnp.float32).reshape(rows, KV_HEADS, groups, HEAD_DIM)
    knew = key_new.astype(jnp.float32).reshape(rows, KV_HEADS, HEAD_DIM)
    vnew = value_new.astype(jnp.float32).reshape(rows, KV_HEADS, HEAD_DIM)
    kcache = cache_keys.astype(jnp.float32)
    vcache = cache_values.astype(jnp.float32)
    valid = (jnp.arange(CACHE, dtype=jnp.int32)[None, :] < lengths[:, None])[:, None, None, :]
    first = jnp.einsum('sgqd,spgd->sgqp', qfull[..., :half], kcache[..., :half]) * scale
    first_own = jnp.einsum('sgqd,sgd->sgq', qfull[..., :half], knew[..., :half]) * scale
    second = jnp.einsum('sgqd,spgd->sgqp', qfull[..., half:], kcache[..., half:]) * scale
    second_own = jnp.einsum('sgqd,sgd->sgq', qfull[..., half:], knew[..., half:]) * scale
    prob_one, own_one = softmax_pair(first, first_own, valid)
    prob_two, own_two = softmax_pair(second, second_own, valid)
    lam = mix_lambda.astype(jnp.float32).reshape(KV_HEADS, groups)
    weights = (prob_one - lam[None, :, :, None] * prob_two).astype(jnp.bfloat16)
    own_weights = (own_one - lam[None] * own_two).astype(jnp.bfloat16)
    mixed = jnp.einsum('sgqp,spgd->sgqd', weights.astype(jnp.float32), vcache)
    mixed = mixed + own_weights.astype(jnp.float32)[..., None] * vnew[:, :, None, :]
    heads = rms_norm(mixed, head_gain, 1e-05).astype(jnp.bfloat16).reshape(rows, HEADS * HEAD_DIM)
    hidden_state = xfull + jnp.dot(heads, out_w, preferred_element_type=jnp.float32)
    ffn_in = rms_norm(hidden_state, ffn_gain, 1e-06).astype(jnp.bfloat16)
    return (hidden_state, ffn_in, key_new, value_new)

def reference(tokens, lengths, cache_keys, cache_values, query_w, key_w, value_w, out_w, mix_lambda, head_gain, attn_gain, ffn_gain, routes, route_weights, exp_gate, exp_up, exp_down, dense_gate, dense_up, dense_down, branch_gate):
    blocks = tokens.shape[0] // SEQ_DEV

    def one_block(pieces):
        return attend_block(pieces[0], pieces[1], pieces[2], pieces[3], query_w, key_w, value_w, out_w, mix_lambda, head_gain, attn_gain, ffn_gain)
    hidden_state, ffn_in, key_new, value_new = lax.map(one_block, (tokens.reshape(blocks, SEQ_DEV, D), lengths.reshape(blocks, SEQ_DEV), cache_keys.reshape(blocks, SEQ_DEV, CACHE, KV_HEADS, HEAD_DIM), cache_values.reshape(blocks, SEQ_DEV, CACHE, KV_HEADS, HEAD_DIM)))
    hidden_state = hidden_state.reshape(TOKENS, D)
    ffn_in = ffn_in.reshape(TOKENS, D)
    key_new = key_new.reshape(TOKENS, KV_HEADS * HEAD_DIM)
    value_new = value_new.reshape(TOKENS, KV_HEADS * HEAD_DIM)
    slots = N_EP * CAP

    def one_expert(total, expert):
        match = routes == expert
        hit = jnp.any(match, axis=-1)
        weight = lax.optimization_barrier(jnp.sum(jnp.where(match, route_weights.astype(jnp.float32), 0.0), axis=-1))
        rank = jnp.cumsum(hit.astype(jnp.int32)) - 1
        select = hit[None, :] & (rank[None, :] == jnp.arange(slots, dtype=jnp.int32)[:, None])
        chosen = jnp.dot(select.astype(jnp.bfloat16), ffn_in, preferred_element_type=jnp.float32).astype(jnp.bfloat16)
        start = (expert * EXP_FF).astype(jnp.int32)
        w_gate = lax.dynamic_slice_in_dim(exp_gate, start, EXP_FF, 1)
        w_up = lax.dynamic_slice_in_dim(exp_up, start, EXP_FF, 1)
        w_down = lax.dynamic_slice_in_dim(exp_down, start, EXP_FF, 0)
        gate_part = jnp.dot(chosen, w_gate, preferred_element_type=jnp.float32)
        up_part = jnp.dot(chosen, w_up, preferred_element_type=jnp.float32)
        act = (jax.nn.silu(gate_part) * up_part).astype(jnp.bfloat16)
        result = jnp.dot(act, w_down, preferred_element_type=jnp.float32)
        back = jnp.dot(select.astype(jnp.float32).T, result, precision=lax.Precision.HIGHEST)
        return (total + weight[:, None] * back, None)
    routed, unused = lax.scan(one_expert, jnp.zeros((TOKENS, D), jnp.float32), jnp.arange(EXPERTS, dtype=jnp.int32))
    row_span = D // BLOCKS
    col_span = DENSE_FF // SPLIT
    gate_full = dense_gate.reshape(BLOCKS, SPLIT, row_span, col_span).transpose(0, 2, 1, 3).reshape(D, DENSE_FF)
    up_full = dense_up.reshape(BLOCKS, SPLIT, row_span, col_span).transpose(0, 2, 1, 3).reshape(D, DENSE_FF)
    down_full = dense_down.reshape(BLOCKS, SPLIT, col_span, row_span).transpose(1, 2, 0, 3).reshape(DENSE_FF, D)
    gate_part = jnp.dot(ffn_in, gate_full, preferred_element_type=jnp.float32)
    up_part = jnp.dot(ffn_in, up_full, preferred_element_type=jnp.float32)
    dense_act = (jax.nn.silu(gate_part) * up_part).astype(jnp.bfloat16)
    dense = jnp.dot(dense_act, down_full, preferred_element_type=jnp.float32)
    gate = jax.nn.sigmoid(jnp.dot(ffn_in, branch_gate, preferred_element_type=jnp.float32))
    output = (hidden_state + routed + gate[:, None] * dense).astype(jnp.bfloat16)
    return (output, key_new, value_new)
```

```python
import functools

import jax
import jax.numpy as jnp
from jax import lax
from jax.experimental import pallas as pl
from jax.experimental.pallas import tpu as pltpu
from jax.sharding import PartitionSpec as P

HEADS = 8
KV_HEADS = 2
HEAD_DIM = 128
SPLIT = 16
BLOCKS = 8
EXPERTS = 8
SIDE = 128
QKV_CHUNKS = 4
T = 4
UNITS = 48
GROUP = 8
COLOURS = (("z", "y", "x"), ("x", "y", "z"), ("y", "z", "x"))
IN_COLS = ((0, 768), (768, 1536), (1536, 2176))
OUT_COLS = ((0, 768), (768, 1408), (1408, 2048))

F32 = jnp.float32
BF16 = jnp.bfloat16
MESH = pl.DeviceIdType.MESH


def loop(low, high, body):
    def run(i, carry):
        body(i)
        return carry

    lax.fori_loop(low, high, run, 0)


def silu(v):
    return v / (1.0 + jnp.exp(-v))


def layer_kernel(
    tokens_h,
    lengths_h,
    lam_h,
    head_gain_h,
    attn_gain_h,
    ffn_gain_h,
    routes_h,
    route_weights_h,
    branch_gate_h,
    keys,
    values,
    query_w,
    key_w,
    value_w,
    out_w,
    exp_gate,
    exp_up,
    exp_down,
    dense_gate,
    dense_up,
    dense_down,
    out,
    new_keys,
    new_values,
    tokens,
    lengths,
    lam,
    head_gain,
    attn_gain,
    ffn_gain,
    routes,
    route_weights,
    branch_gate,
    small_sem,
    ext,
    hidden,
    kbuf,
    vbuf,
    qbuf,
    kwbuf,
    vwbuf,
    obuf,
    qscr,
    hscr,
    qkv_sem,
    ksem,
    vsem,
    osem,
    ew,
    dn,
    dgw,
    duw,
    w_sem,
    ws_send,
    ws_recv,
    ds_send,
    ds_recv,
    df_send,
    df_recv,
    recv0,
    recv1,
    recv2,
    side,
    xall,
    act,
    act_perm,
    perm,
    total,
    sendb0,
    sendb1,
    sendb2,
    recvb0,
    recvb1,
    recvb2,
    senda0,
    senda1,
    senda2,
    recva0,
    recva1,
    recva2,
    aga_send,
    aga_recv,
    agb_send,
    agb_recv,
    rsb_send,
    rsb_recv,
    rsa_send,
    rsa_recv,
):
    recv = (recv0, recv1, recv2)
    sendb, recvb = (sendb0, sendb1, sendb2), (recvb0, recvb1, recvb2)
    senda, recva = (senda0, senda1, senda2), (recva0, recva1, recva2)
    rows, width = tokens.shape
    ffn_cols = exp_gate.shape[1]
    all_rows = xall.shape[0]
    span = keys.shape[1]
    step = width // QKV_CHUNKS
    heads_of = HEADS // KV_HEADS
    half = HEAD_DIM // 2
    block_cols = width // BLOCKS

    me = lax.axis_index("ep")
    core = lax.rem(me, 2)
    chip = me // 2
    place = {"z": chip // (T * T), "y": lax.rem(chip // T, T), "x": lax.rem(chip, T)}
    block = me // SPLIT
    expert = block

    def device(at):
        return ((at["z"] * T + at["y"]) * T + at["x"]) * 2 + core

    def mate(c, da, dp, dq):
        at = {name: lax.rem(place[name] + d, T) for name, d in zip(COLOURS[c], (da, dp, dq))}
        return device(at)

    sibling = chip * 2 + 1 - core

    small = [
        pltpu.make_async_copy(src, dst, small_sem.at[i])
        for i, (src, dst) in enumerate(
            (
                (tokens_h, tokens),
                (attn_gain_h, attn_gain),
                (lengths_h, lengths),
                (lam_h, lam),
                (head_gain_h, head_gain),
                (ffn_gain_h, ffn_gain),
                (routes_h, routes),
                (route_weights_h, route_weights),
                (branch_gate_h, branch_gate),
            )
        )
    ]
    for copy in small:
        copy.start()
    weight_copies = []
    for c in range(QKV_CHUNKS):
        part = pl.ds(c * step, step)
        trio = [
            pltpu.make_async_copy(src.at[part], dst.at[part], qkv_sem.at[3 * c + i])
            for i, (src, dst) in enumerate(((query_w, qbuf), (key_w, kwbuf), (value_w, vwbuf)))
        ]
        for copy in trio:
            copy.start()
        weight_copies.append(trio)
    key_copies = [pltpu.make_async_copy(keys.at[s], kbuf.at[s], ksem.at[s]) for s in range(rows)]
    value_copies = [pltpu.make_async_copy(values.at[s], vbuf.at[s], vsem.at[s]) for s in range(rows)]
    for s in range(rows):
        key_copies[s].start()
        value_copies[s].start()
    out_copy = pltpu.make_async_copy(out_w, obuf, osem.at[0])
    out_copy.start()

    gate_cols = pl.ds(pl.multiple_of(core * ffn_cols, 128), ffn_cols)
    up_cols = pl.ds(pl.multiple_of((2 + core) * ffn_cols, 128), ffn_cols)
    down_rows = pl.ds(pl.multiple_of(core * ffn_cols, 128), ffn_cols)
    tile_rows = pl.ds(pl.multiple_of(core * UNITS, 16), UNITS)
    tile_down_rows = pl.ds(pl.multiple_of(2 * ffn_cols + core * UNITS, 16), UNITS)
    tile_cols = pl.ds(pl.multiple_of(block * block_cols, 128), block_cols)

    def window(b):
        return pl.ds(pl.multiple_of(((11 * b) // 2) * GROUP, GROUP), UNITS)

    own_loads = [
        pltpu.make_async_copy(src, dst, w_sem.at[i])
        for i, (src, dst) in enumerate(
            (
                (dense_gate.at[0, window(block)], dgw.at[block, tile_rows]),
                (dense_up.at[0, window(block)], duw.at[block, tile_rows]),
                (dense_down.at[0, window(block)], dn.at[tile_down_rows, tile_cols]),
                (exp_gate, ew.at[:, gate_cols]),
                (exp_up, ew.at[:, up_cols]),
                (exp_down, dn.at[down_rows]),
            )
        )
    ]
    for copy in own_loads:
        copy.start()

    barrier = pltpu.get_barrier_semaphore()
    greeted = 0
    for dz in range(T):
        for dy in range(T):
            for dx in range(T):
                if (dz == 0 or dy == 0 or dx == 0) and (dz, dy, dx) != (0, 0, 0):
                    at = {
                        "z": lax.rem(place["z"] + dz, T),
                        "y": lax.rem(place["y"] + dy, T),
                        "x": lax.rem(place["x"] + dx, T),
                    }
                    pl.semaphore_signal(barrier, inc=1, device_id=(device(at),), device_id_type=MESH)
                    greeted += 1
    pl.semaphore_signal(barrier, inc=1, device_id=(sibling,), device_id_type=MESH)
    greeted += 1

    want = lax.broadcasted_iota(jnp.int32, (all_rows, all_rows), 0)
    have = lax.broadcasted_iota(jnp.int32, (all_rows, all_rows), 1)
    low = have & 3
    first, second, third = (have >> 2) & 3, (have >> 4) & 3, have >> 6
    perm[...] = jnp.where(want == ((first << 6) + (second << 4) + (third << 2) + low), 1.0, 0.0).astype(BF16)
    pad = act.shape[1] - 2 * ffn_cols - 2 * UNITS
    act[:, 2 * ffn_cols + 2 * UNITS :] = jnp.zeros((all_rows, pad), BF16)
    dn[2 * ffn_cols + 2 * UNITS :, :] = jnp.zeros((pad, width), BF16)

    for copy in small:
        copy.wait()

    x = tokens[...].astype(F32)
    normed = x * lax.rsqrt(jnp.mean(x * x, axis=-1, keepdims=True) + 1e-06) * attn_gain[...]
    normed = normed.astype(BF16)
    query = jnp.zeros((rows, query_w.shape[1]), F32)
    knew = jnp.zeros((rows, key_w.shape[1]), F32)
    vnew = jnp.zeros((rows, value_w.shape[1]), F32)
    for c in range(QKV_CHUNKS):
        for copy in weight_copies[c]:
            copy.wait()
        part = slice(c * step, (c + 1) * step)
        left = normed[:, part]
        query += jnp.dot(left, qbuf[part, :], preferred_element_type=F32)
        knew += jnp.dot(left, kwbuf[part, :], preferred_element_type=F32)
        vnew += jnp.dot(left, vwbuf[part, :], preferred_element_type=F32)
    new_keys[...] = knew.astype(BF16)
    new_values[...] = vnew.astype(BF16)
    query = query.astype(BF16).astype(F32)
    knew = knew.astype(BF16).astype(F32)
    vnew = vnew.astype(BF16).astype(F32)
    for s in range(rows):
        for h in range(HEADS):
            qscr[s, h : h + 1, :] = query[s : s + 1, h * HEAD_DIM : (h + 1) * HEAD_DIM]

    pl.semaphore_wait(barrier, greeted)

    def tile_copies(j):
        target = lax.rem(block + j, BLOCKS)
        peer = target * SPLIT + lax.rem(me, SPLIT)
        return [
            pltpu.make_async_remote_copy(
                src_ref=src.at[0, window(target)],
                dst_ref=dst,
                send_sem=ds_send.at[3 * j + i],
                recv_sem=ds_recv.at[3 * j + i],
                device_id=(peer,),
                device_id_type=MESH,
            )
            for i, (src, dst) in enumerate(
                (
                    (dense_gate, dgw.at[block, tile_rows]),
                    (dense_up, duw.at[block, tile_rows]),
                    (dense_down, dn.at[tile_down_rows, tile_cols]),
                )
            )
        ]

    def to_sibling(src, dst, send, recv_sem):
        return pltpu.make_async_remote_copy(
            src_ref=src, dst_ref=dst, send_sem=send, recv_sem=recv_sem, device_id=(sibling,), device_id_type=MESH
        )

    expert_copies = [
        to_sibling(src, dst, ws_send.at[i], ws_recv.at[i])
        for i, (src, dst) in enumerate(
            ((exp_gate, ew.at[:, gate_cols]), (exp_up, ew.at[:, up_cols]), (exp_down, dn.at[down_rows]))
        )
    ]
    tile_forwards = [
        to_sibling(ref, ref, df_send.at[i], df_recv.at[i])
        for i, ref in enumerate((dgw.at[:, tile_rows], duw.at[:, tile_rows], dn.at[tile_down_rows]))
    ]
    for j in range(1, BLOCKS):
        for copy in tile_copies(j):
            copy.start()
    for copy in expert_copies:
        copy.start()

    scale = half ** (-0.5)
    lane = lax.broadcasted_iota(jnp.int32, (HEADS, HEAD_DIM), 1)
    head_row = lax.broadcasted_iota(jnp.int32, (HEADS, HEAD_DIM), 0)
    col = lax.broadcasted_iota(jnp.int32, (2 * HEADS, span), 1)
    row = lax.broadcasted_iota(jnp.int32, (2 * HEADS, span), 0)
    own_group = (col % KV_HEADS) == ((row % HEADS) // heads_of)
    head_col = lax.broadcasted_iota(jnp.int32, (HEADS, 1), 0)
    lam_col = jnp.zeros((HEADS, 1), F32)
    for h in range(HEADS):
        lam_col = jnp.where(head_col == h, lam[h], lam_col)
    for s in range(rows):
        q = qscr[s]
        both = jnp.concatenate([jnp.where(lane < half, q, 0.0), jnp.where(lane >= half, q, 0.0)], axis=0)
        kown = jnp.zeros((HEADS, HEAD_DIM), F32)
        vown = jnp.zeros((HEADS, HEAD_DIM), F32)
        for g in range(KV_HEADS):
            mine = head_row // heads_of == g
            part = slice(g * HEAD_DIM, (g + 1) * HEAD_DIM)
            kown = jnp.where(mine, knew[s : s + 1, part], kown)
            vown = jnp.where(mine, vnew[s : s + 1, part], vown)
        own = jnp.sum(both * jnp.concatenate([kown, kown], axis=0), axis=-1, keepdims=True) * scale
        key_copies[s].wait()
        scores = lax.dot_general(
            both.astype(BF16), kbuf[s], (((1,), (1,)), ((), ())), preferred_element_type=F32
        ) * scale
        valid = own_group & (col < KV_HEADS * lengths[s])
        largest = jnp.maximum(jnp.max(jnp.where(valid, scores, -jnp.inf), axis=-1, keepdims=True), own)
        raised = jnp.where(valid, jnp.exp(scores - largest), 0.0)
        own_raised = jnp.exp(own - largest)
        inverse = 1.0 / (jnp.sum(raised, axis=-1, keepdims=True) + own_raised)
        prob = raised * inverse
        own_prob = own_raised * inverse
        weights = (prob[:HEADS] - lam_col * prob[HEADS:]).astype(BF16)
        own_weights = (own_prob[:HEADS] - lam_col * own_prob[HEADS:]).astype(BF16).astype(F32)
        value_copies[s].wait()
        mixed = jnp.dot(weights, vbuf[s], preferred_element_type=F32) + own_weights * vown
        normal = mixed * lax.rsqrt(jnp.mean(mixed * mixed, axis=-1, keepdims=True) + 1e-05)
        normal = normal * head_gain[...]
        for h in range(HEADS):
            hscr[s : s + 1, h * HEAD_DIM : (h + 1) * HEAD_DIM] = normal[h : h + 1, :]
    out_copy.wait()
    state = x + jnp.dot(hscr[...].astype(BF16), obuf[...], preferred_element_type=F32)
    hidden[...] = state
    ffn = state * lax.rsqrt(jnp.mean(state * state, axis=-1, keepdims=True) + 1e-06)
    ffn = (ffn * ffn_gain[...]).astype(BF16)
    ext[:, :width] = ffn
    pieces = jnp.zeros((rows, SIDE), F32)
    branch = branch_gate[...].astype(F32)
    for c in range(width // SIDE):
        pieces += ffn[:, c * SIDE : (c + 1) * SIDE].astype(F32) * branch[c : c + 1, :]
    logit = jnp.sum(pieces, axis=-1, keepdims=True)
    gate = 1.0 / (1.0 + jnp.exp(-logit))
    spot = lax.broadcasted_iota(jnp.int32, (rows, SIDE), 1)
    name = spot % (SIDE // 2)
    table = jnp.where(name == EXPERTS, gate, 0.0)
    token_row = lax.broadcasted_iota(jnp.int32, (rows, SIDE), 0)
    for k in range(routes.shape[0]):
        for s in range(rows):
            here = (name == routes[k, s]) & (name < EXPERTS) & (token_row == s)
            table = table + jnp.where(here, route_weights[k, s], 0.0)
    high = table.astype(BF16).astype(F32)
    ext[:, width:] = jnp.where(spot < SIDE // 2, high, table - high).astype(BF16)

    def spots(c):
        return [place[name] for name in COLOURS[c]]

    def plane_send(c, dp, dq):
        a, p, q = spots(c)
        i = (c * T + dp) * T + dq
        first, last = IN_COLS[c]
        return pltpu.make_async_remote_copy(
            src_ref=ext.at[:, first:last],
            dst_ref=recv[c].at[(a * T + p) * T + q],
            send_sem=aga_send.at[i],
            recv_sem=aga_recv.at[i],
            device_id=(mate(c, 0, dp, dq),),
            device_id_type=MESH,
        )

    def axis_send(c, da, dp):
        a, p, q = spots(c)
        from_p = lax.rem(p + T - dp, T)
        piece = recv[c].at[pl.ds((a * T + from_p) * T, T)]
        i = (c * (T - 1) + da - 1) * T + dp
        return pltpu.make_async_remote_copy(
            src_ref=piece,
            dst_ref=piece,
            send_sem=agb_send.at[i],
            recv_sem=agb_recv.at[i],
            device_id=(mate(c, da, 0, 0),),
            device_id_type=MESH,
        )

    for dp in (2, 1, 3, 0):
        for dq in (2, 1, 3, 0):
            if (dp, dq) != (0, 0):
                for c in range(3):
                    plane_send(c, dp, dq).start()
    for c in range(3):
        a, p, q = spots(c)
        first, last = IN_COLS[c]
        recv[c][(a * T + p) * T + q] = ext[:, first:last]
    for dp in (0, 1, 3, 2):
        for c in range(3):
            for dq in range(T):
                if (dp, dq) != (0, 0):
                    plane_send(c, dp, dq).wait_recv()
            for da in (2, 1, 3):
                axis_send(c, da, dp).start()
    for copy in own_loads[:3]:
        copy.wait()
    for j in range(1, BLOCKS):
        for copy in tile_copies(j):
            copy.wait_recv()
    for copy in tile_forwards:
        copy.start()

    def widen(z, y):
        group = z * T + y
        at = pl.ds(pl.multiple_of(group * 16, 16), 16)

        def four(ref, spots_of, cols):
            return jnp.concatenate([ref[i, :, cols].astype(F32) for i in spots_of], axis=0)

        one = four(recv0, [group * T + i for i in range(T)], slice(None))
        xall[at, IN_COLS[0][0] : IN_COLS[0][1]] = one.astype(BF16)
        one = four(recv1, [(i * T + y) * T + z for i in range(T)], slice(None))
        xall[at, IN_COLS[1][0] : IN_COLS[1][1]] = one.astype(BF16)
        where = [(y * T + z) * T + i for i in range(T)]
        one = four(recv2, where, slice(0, width - IN_COLS[2][0]))
        xall[at, IN_COLS[2][0] : width] = one.astype(BF16)
        side[at, :] = four(recv2, where, slice(width - IN_COLS[2][0], None))

    for da in (1, 3, 2):
        for dp in (0, 1, 3, 2):
            for c in range(3):
                axis_send(c, da, dp).wait_recv()
    loop(0, T * T, lambda i: widen(i // T, lax.rem(i, T)))

    for copy in own_loads[3:]:
        copy.wait()
    for copy in expert_copies:
        copy.wait_recv()

    spot = lax.broadcasted_iota(jnp.int32, side.shape, 1) % (SIDE // 2)
    table = side[...]
    routed = jnp.sum(jnp.where(spot == expert, table, 0.0), axis=-1, keepdims=True)
    gate = jnp.sum(jnp.where(spot == EXPERTS, table, 0.0), axis=-1, keepdims=True)
    hid = 2 * ffn_cols
    for n in range(hid // 256):
        cols = slice(n * 256, (n + 1) * 256)
        g = jnp.dot(xall[...], ew[:, cols], preferred_element_type=F32)
        u = jnp.dot(xall[...], ew[:, hid + n * 256 : hid + (n + 1) * 256], preferred_element_type=F32)
        act[:, cols] = (silu(g) * u * routed).astype(BF16)
    for copy in tile_forwards:
        copy.wait_recv()
    across = (((1,), (1,)), ((), ()))
    g = jnp.zeros((all_rows, 2 * UNITS), F32)
    u = jnp.zeros((all_rows, 2 * UNITS), F32)
    for b in range(BLOCKS):
        left = xall[:, b * block_cols : (b + 1) * block_cols]
        g += lax.dot_general(left, dgw[b], across, preferred_element_type=F32)
        u += lax.dot_general(left, duw[b], across, preferred_element_type=F32)
    unit = lax.broadcasted_iota(jnp.int32, g.shape, 1)
    unit = jnp.where(unit >= UNITS, unit - UNITS, unit)
    taken = UNITS - GROUP * (1 - lax.rem(block, 2))
    dact = jnp.where(unit < taken, silu(g) * u * gate, 0.0)
    act[:, hid : hid + 2 * UNITS] = dact.astype(BF16)
    act_perm[...] = jnp.dot(perm[...], act[...], preferred_element_type=F32).astype(BF16)

    def slab(c, a, p):
        return p * T + a if c == 2 else a * T + p

    def axis_sum(c, da, k):
        a, p, q = spots(c)
        i = (c * (T - 1) + da - 1) * T + k
        return pltpu.make_async_remote_copy(
            src_ref=sendb[c].at[slab(c, lax.rem(a + da, T), lax.rem(p + k, T))],
            dst_ref=recvb[c].at[(da - 1) * T + k],
            send_sem=rsb_send.at[i],
            recv_sem=rsb_recv.at[i],
            device_id=(mate(c, da, 0, 0),),
            device_id_type=MESH,
        )

    def plane_sum(c, k, l):
        a, p, q = spots(c)
        i = (c * T + k) * T + l
        return pltpu.make_async_remote_copy(
            src_ref=senda[c].at[lax.rem(p + k, T) * T + lax.rem(q + l, T)],
            dst_ref=recva[c].at[k * T + l],
            send_sem=rsa_send.at[i],
            recv_sem=rsa_recv.at[i],
            device_id=(mate(c, 0, k, l),),
            device_id_type=MESH,
        )

    for c in range(3):
        first, last = OUT_COLS[c]
        left = act_perm if c == 1 else act
        part = jnp.dot(left[...], dn[:, first:last], preferred_element_type=F32)
        total[:, first:last] = part
        for i in range(T * T):
            sendb[c][i] = part[i * 16 : (i + 1) * 16].astype(BF16)
        for k in (2, 1, 3, 0):
            for da in (2, 1, 3):
                axis_sum(c, da, k).start()

    for c in range(3):
        for dp in range(T):
            for dq in range(T):
                if (dp, dq) != (0, 0):
                    plane_send(c, dp, dq).wait_send()
        for da in range(1, T):
            for dp in range(T):
                axis_send(c, da, dp).wait_send()
    for j in range(1, BLOCKS):
        for copy in tile_copies(j):
            copy.wait_send()
    for copy in expert_copies:
        copy.wait_send()
    for copy in tile_forwards:
        copy.wait_send()

    for k in (2, 1, 3, 0):
        for c in range(3):
            a, p, q = spots(c)
            first, last = OUT_COLS[c]
            row16 = pl.ds(pl.multiple_of(slab(c, a, lax.rem(p + k, T)) * 16, 16), 16)
            acc = total[row16, first:last]
            for da in (1, 3, 2):
                axis_sum(c, da, k).wait_recv()
                acc = acc + recvb[c][(da - 1) * T + k].astype(F32)
            for i in range(T):
                senda[c][lax.rem(p + k, T) * T + i] = acc[i * rows : (i + 1) * rows].astype(BF16)
            for l in (2, 1, 3, 0):
                if (k, l) != (0, 0):
                    plane_sum(c, k, l).start()
    for c in range(3):
        for da in range(1, T):
            for k in range(T):
                axis_sum(c, da, k).wait_send()
    for c in range(3):
        a, p, q = spots(c)
        first, last = OUT_COLS[c]
        acc = hidden[:, first:last] + senda[c][p * T + q].astype(F32)
        for k in (0, 1, 3, 2):
            for l in (0, 1, 3, 2):
                if (k, l) != (0, 0):
                    plane_sum(c, k, l).wait_recv()
                    acc = acc + recva[c][k * T + l].astype(F32)
        out[:, first:last] = acc.astype(BF16)
    for c in range(3):
        for k in range(T):
            for l in range(T):
                if (k, l) != (0, 0):
                    plane_sum(c, k, l).wait_send()


def finish_kernel(count, *refs):
    sources, targets, held = refs[:count], refs[count : 2 * count], refs[2 * count : 3 * count]
    in_sem, out_sem = refs[3 * count :]
    ins = [pltpu.make_async_copy(sources[i], held[i], in_sem.at[i]) for i in range(count)]
    outs = [pltpu.make_async_copy(held[i], targets[i], out_sem.at[i]) for i in range(count)]
    for copy in ins:
        copy.start()
    for i in range(count):
        ins[i].wait()
        outs[i].start()
    for copy in outs:
        copy.wait()


def per_device(
    tokens,
    lengths,
    cache_keys,
    cache_values,
    query_w,
    key_w,
    value_w,
    out_w,
    mix_lambda,
    head_gain,
    attn_gain,
    ffn_gain,
    routes,
    route_weights,
    exp_gate,
    exp_up,
    exp_down,
    dense_gate,
    dense_up,
    dense_down,
    branch_gate,
):
    rows, width = tokens.shape
    span = cache_keys.shape[1] * KV_HEADS
    vmem = pl.BlockSpec(memory_space=pltpu.VMEM)
    anywhere = pl.BlockSpec(memory_space=pl.ANY)
    chips = T * T * T
    all_rows = chips * rows
    hid = 2 * exp_gate.shape[1]
    padded = -(-(hid + 2 * UNITS) // 128) * 128
    block_cols = width // BLOCKS
    sem = pltpu.SemaphoreType.DMA
    dense_gate = jnp.swapaxes(dense_gate, 1, 2)
    dense_up = jnp.swapaxes(dense_up, 1, 2)
    routes = routes.T
    route_weights = route_weights.T
    in_cols = [last - first for first, last in IN_COLS]
    out_cols = [last - first for first, last in OUT_COLS]
    results = pl.pallas_call(
        layer_kernel,
        name="layer",
        out_shape=(
            jax.ShapeDtypeStruct((rows, width), BF16),
            jax.ShapeDtypeStruct((rows, key_w.shape[1]), BF16),
            jax.ShapeDtypeStruct((rows, value_w.shape[1]), BF16),
        ),
        in_specs=[anywhere] * 21,
        out_specs=(vmem,) * 3,
        scratch_shapes=[
            pltpu.VMEM((rows, width), BF16),
            pltpu.SMEM(lengths.shape, jnp.int32),
            pltpu.SMEM(mix_lambda.shape, F32),
            pltpu.VMEM((1, HEAD_DIM), F32),
            pltpu.VMEM((1, width), F32),
            pltpu.VMEM((1, width), F32),
            pltpu.SMEM(routes.shape, jnp.int32),
            pltpu.SMEM(route_weights.shape, F32),
            pltpu.VMEM((width // SIDE, SIDE), BF16),
            sem((9,)),
            pltpu.VMEM((rows, width + SIDE), BF16),
            pltpu.VMEM((rows, width), F32),
            pltpu.VMEM((rows, span, HEAD_DIM), BF16),
            pltpu.VMEM((rows, span, HEAD_DIM), BF16),
            pltpu.VMEM(query_w.shape, BF16),
            pltpu.VMEM(key_w.shape, BF16),
            pltpu.VMEM(value_w.shape, BF16),
            pltpu.VMEM(out_w.shape, BF16),
            pltpu.VMEM((rows, HEADS, HEAD_DIM), F32),
            pltpu.VMEM((rows, HEADS * HEAD_DIM), F32),
            sem((3 * QKV_CHUNKS,)),
            sem((rows,)),
            sem((rows,)),
            sem((1,)),
            pltpu.VMEM((width, 2 * hid), BF16),
            pltpu.VMEM((padded, width), BF16),
            pltpu.VMEM((BLOCKS, 2 * UNITS, block_cols), BF16),
            pltpu.VMEM((BLOCKS, 2 * UNITS, block_cols), BF16),
            sem((6,)),
            sem((3,)),
            sem((3,)),
            sem((3 * BLOCKS,)),
            sem((3 * BLOCKS,)),
            sem((3,)),
            sem((3,)),
        ]
        + [pltpu.VMEM((chips, rows, cols), BF16) for cols in in_cols]
        + [
            pltpu.VMEM((all_rows, SIDE), F32),
            pltpu.VMEM((all_rows, width), BF16),
            pltpu.VMEM((all_rows, padded), BF16),
            pltpu.VMEM((all_rows, padded), BF16),
            pltpu.VMEM((all_rows, all_rows), BF16),
            pltpu.VMEM((all_rows, width), F32),
        ]
        + [pltpu.VMEM((T * T, T * rows, cols), BF16) for cols in out_cols]
        + [pltpu.VMEM(((T - 1) * T, T * rows, cols), BF16) for cols in out_cols]
        + [pltpu.VMEM((T * T, rows, cols), BF16) for cols in out_cols]
        + [pltpu.VMEM((T * T, rows, cols), BF16) for cols in out_cols]
        + [
            sem((3 * T * T,)),
            sem((3 * T * T,)),
            sem((3 * (T - 1) * T,)),
            sem((3 * (T - 1) * T,)),
            sem((3 * (T - 1) * T,)),
            sem((3 * (T - 1) * T,)),
            sem((3 * T * T,)),
            sem((3 * T * T,)),
        ],
        compiler_params=pltpu.CompilerParams(
            collective_id=0, has_side_effects=True, vmem_limit_bytes=63 * 2**20
        ),
    )(
        tokens,
        lengths,
        mix_lambda,
        head_gain.reshape(1, HEAD_DIM),
        attn_gain.reshape(1, width),
        ffn_gain.reshape(1, width),
        routes,
        route_weights,
        branch_gate.reshape(width // SIDE, SIDE),
        cache_keys.reshape(rows, span, HEAD_DIM),
        cache_values.reshape(rows, span, HEAD_DIM),
        query_w,
        key_w,
        value_w,
        out_w,
        exp_gate,
        exp_up,
        exp_down,
        dense_gate,
        dense_up,
        dense_down,
    )
    count = len(results)
    return pl.pallas_call(
        functools.partial(finish_kernel, count),
        name="finish",
        out_shape=tuple(jax.ShapeDtypeStruct(r.shape, r.dtype) for r in results),
        in_specs=[anywhere] * count,
        out_specs=(anywhere,) * count,
        scratch_shapes=[pltpu.VMEM(r.shape, r.dtype) for r in results] + [sem((count,)), sem((count,))],
        compiler_params=pltpu.CompilerParams(vmem_limit_bytes=63 * 2**20),
    )(*results)


def solution(mesh):
    placed = (
        P("ep", None),
        P("ep"),
        P("ep", None, None, None),
        P("ep", None, None, None),
        P(),
        P(),
        P(),
        P(),
        P(),
        P(),
        P(),
        P(),
        P("ep", None),
        P("ep", None),
        P(None, "ep"),
        P(None, "ep"),
        P("ep", None),
        P("ep", None, None),
        P("ep", None, None),
        P("ep", None, None),
        P(),
    )
    return jax.shard_map(
        per_device,
        mesh=mesh,
        in_specs=placed,
        out_specs=(P("ep", None), P("ep", None), P("ep", None)),
        check_vma=False,
    )
```

```python
import functools

import jax
import jax.numpy as jnp
from jax import lax
from jax.experimental import pallas as pl
from jax.experimental.pallas import tpu as pltpu
from jax.sharding import PartitionSpec as P

HEADS = 8
KV_HEADS = 2
HEAD_DIM = 128
SPLIT = 16
BLOCKS = 8
EXPERTS = 8
SIDE = 128
QKV_CHUNKS = 4
T = 4
UNITS = 48
GROUP = 8
COLOURS = (("z", "y", "x"), ("x", "y", "z"), ("y", "z", "x"))
IN_COLS = ((0, 768), (768, 1536), (1536, 2176))
OUT_COLS = ((0, 768), (768, 1408), (1408, 2048))

F32 = jnp.float32
BF16 = jnp.bfloat16
MESH = pl.DeviceIdType.MESH


def loop(low, high, body):
    def run(i, carry):
        body(i)
        return carry

    lax.fori_loop(low, high, run, 0)


def silu(v):
    return v / (1.0 + jnp.exp(-v))


def layer_kernel(
    tokens_h,
    lengths_h,
    lam_h,
    head_gain_h,
    attn_gain_h,
    ffn_gain_h,
    routes_h,
    route_weights_h,
    branch_gate_h,
    keys,
    values,
    query_w,
    key_w,
    value_w,
    out_w,
    exp_gate,
    exp_up,
    exp_down,
    dense_gate,
    dense_up,
    dense_down,
    out,
    new_keys,
    new_values,
    tokens,
    lengths,
    lam,
    head_gain,
    attn_gain,
    ffn_gain,
    routes,
    route_weights,
    branch_gate,
    small_sem,
    ext,
    hidden,
    kbuf,
    vbuf,
    qbuf,
    kwbuf,
    vwbuf,
    obuf,
    qscr,
    hscr,
    qkv_sem,
    ksem,
    vsem,
    osem,
    ew,
    dn,
    dgw,
    duw,
    w_sem,
    ws_send,
    ws_recv,
    ds_send,
    ds_recv,
    df_send,
    df_recv,
    recv0,
    recv1,
    recv2,
    side,
    xall,
    act,
    act_perm,
    perm,
    sendb0,
    sendb1,
    sendb2,
    recvb0,
    recvb1,
    recvb2,
    senda0,
    senda1,
    senda2,
    recva0,
    recva1,
    recva2,
    aga_send,
    aga_recv,
    agb_send,
    agb_recv,
    rsb_send,
    rsb_recv,
    rsa_send,
    rsa_recv,
):
    recv = (recv0, recv1, recv2)
    sendb, recvb = (sendb0, sendb1, sendb2), (recvb0, recvb1, recvb2)
    senda, recva = (senda0, senda1, senda2), (recva0, recva1, recva2)
    rows, width = tokens.shape
    ffn_cols = exp_gate.shape[1]
    all_rows = xall.shape[0]
    span = keys.shape[1]
    step = width // QKV_CHUNKS
    heads_of = HEADS // KV_HEADS
    half = HEAD_DIM // 2
    block_cols = width // BLOCKS

    me = lax.axis_index("ep")
    core = lax.rem(me, 2)
    chip = me // 2
    place = {"z": chip // (T * T), "y": lax.rem(chip // T, T), "x": lax.rem(chip, T)}
    block = me // SPLIT
    expert = block

    def device(at):
        return ((at["z"] * T + at["y"]) * T + at["x"]) * 2 + core

    def mate(c, da, dp, dq):
        at = {name: lax.rem(place[name] + d, T) for name, d in zip(COLOURS[c], (da, dp, dq))}
        return device(at)

    sibling = chip * 2 + 1 - core

    small = [
        pltpu.make_async_copy(src, dst, small_sem.at[i])
        for i, (src, dst) in enumerate(
            (
                (tokens_h, tokens),
                (attn_gain_h, attn_gain),
                (lengths_h, lengths),
                (lam_h, lam),
                (head_gain_h, head_gain),
                (ffn_gain_h, ffn_gain),
                (routes_h, routes),
                (route_weights_h, route_weights),
                (branch_gate_h, branch_gate),
            )
        )
    ]
    for copy in small:
        copy.start()
    weight_copies = []
    for c in range(QKV_CHUNKS):
        part = pl.ds(c * step, step)
        trio = [
            pltpu.make_async_copy(src.at[part], dst.at[part], qkv_sem.at[3 * c + i])
            for i, (src, dst) in enumerate(((query_w, qbuf), (key_w, kwbuf), (value_w, vwbuf)))
        ]
        for copy in trio:
            copy.start()
        weight_copies.append(trio)
    key_copies = [pltpu.make_async_copy(keys.at[s], kbuf.at[s], ksem.at[s]) for s in range(rows)]
    value_copies = [pltpu.make_async_copy(values.at[s], vbuf.at[s], vsem.at[s]) for s in range(rows)]
    out_copy = pltpu.make_async_copy(out_w, obuf, osem.at[0])

    gate_cols = pl.ds(pl.multiple_of(core * ffn_cols, 128), ffn_cols)
    up_cols = pl.ds(pl.multiple_of((2 + core) * ffn_cols, 128), ffn_cols)
    down_rows = pl.ds(pl.multiple_of(core * ffn_cols, 128), ffn_cols)
    tile_rows = pl.ds(pl.multiple_of(core * UNITS, 16), UNITS)
    tile_down_rows = pl.ds(pl.multiple_of(2 * ffn_cols + core * UNITS, 16), UNITS)
    tile_cols = pl.ds(pl.multiple_of(block * block_cols, 128), block_cols)

    def window(b):
        return pl.ds(pl.multiple_of(((11 * b) // 2) * GROUP, GROUP), UNITS)

    own_loads = [
        pltpu.make_async_copy(src, dst, w_sem.at[i])
        for i, (src, dst) in enumerate(
            (
                (dense_gate.at[0, window(block)], dgw.at[block, tile_rows]),
                (dense_up.at[0, window(block)], duw.at[block, tile_rows]),
                (dense_down.at[0, window(block)], dn.at[tile_down_rows, tile_cols]),
                (exp_gate, ew.at[:, gate_cols]),
                (exp_up, ew.at[:, up_cols]),
                (exp_down, dn.at[down_rows]),
            )
        )
    ]

    barrier = pltpu.get_barrier_semaphore()
    greeted = 0
    for dz in range(T):
        for dy in range(T):
            for dx in range(T):
                if (dz == 0 or dy == 0 or dx == 0) and (dz, dy, dx) != (0, 0, 0):
                    at = {
                        "z": lax.rem(place["z"] + dz, T),
                        "y": lax.rem(place["y"] + dy, T),
                        "x": lax.rem(place["x"] + dx, T),
                    }
                    pl.semaphore_signal(barrier, inc=1, device_id=(device(at),), device_id_type=MESH)
                    greeted += 1
    pl.semaphore_signal(barrier, inc=1, device_id=(sibling,), device_id_type=MESH)
    greeted += 1

    want = lax.broadcasted_iota(jnp.int32, (all_rows, all_rows), 0)
    have = lax.broadcasted_iota(jnp.int32, (all_rows, all_rows), 1)
    low = have & 3
    first, second, third = (have >> 2) & 3, (have >> 4) & 3, have >> 6
    perm[...] = jnp.where(want == ((first << 6) + (second << 4) + (third << 2) + low), 1.0, 0.0).astype(BF16)
    pad = act.shape[1] - 2 * ffn_cols - 2 * UNITS
    act[:, 2 * ffn_cols + 2 * UNITS :] = jnp.zeros((all_rows, pad), BF16)
    dn[2 * ffn_cols + 2 * UNITS :, :] = jnp.zeros((pad, width), BF16)

    small[0].wait()
    small[1].wait()
    for copy in key_copies + value_copies:
        copy.start()
    x = tokens[...].astype(F32)
    normed = x * lax.rsqrt(jnp.mean(x * x, axis=-1, keepdims=True) + 1e-06) * attn_gain[...]
    normed = normed.astype(BF16)
    query = jnp.zeros((rows, query_w.shape[1]), F32)
    knew = jnp.zeros((rows, key_w.shape[1]), F32)
    vnew = jnp.zeros((rows, value_w.shape[1]), F32)
    for c in range(QKV_CHUNKS):
        for copy in weight_copies[c]:
            copy.wait()
        part = slice(c * step, (c + 1) * step)
        left = normed[:, part]
        query += jnp.dot(left, qbuf[part, :], preferred_element_type=F32)
        knew += jnp.dot(left, kwbuf[part, :], preferred_element_type=F32)
        vnew += jnp.dot(left, vwbuf[part, :], preferred_element_type=F32)
    new_keys[...] = knew.astype(BF16)
    new_values[...] = vnew.astype(BF16)
    query = query.astype(BF16).astype(F32)
    knew = knew.astype(BF16).astype(F32)
    vnew = vnew.astype(BF16).astype(F32)
    for s in range(rows):
        for h in range(HEADS):
            qscr[s, h : h + 1, :] = query[s : s + 1, h * HEAD_DIM : (h + 1) * HEAD_DIM]

    out_copy.start()
    for copy in own_loads:
        copy.start()
    pl.semaphore_wait(barrier, greeted)

    def tile_copies(j):
        target = lax.rem(block + j, BLOCKS)
        peer = target * SPLIT + lax.rem(me, SPLIT)
        return [
            pltpu.make_async_remote_copy(
                src_ref=src.at[0, window(target)],
                dst_ref=dst,
                send_sem=ds_send.at[i],
                recv_sem=ds_recv.at[i],
                device_id=(peer,),
                device_id_type=MESH,
            )
            for i, (src, dst) in enumerate(
                (
                    (dense_gate, dgw.at[block, tile_rows]),
                    (dense_up, duw.at[block, tile_rows]),
                    (dense_down, dn.at[tile_down_rows, tile_cols]),
                )
            )
        ]

    def stand_in(ref, send, recv_sem):
        return pltpu.make_async_remote_copy(
            src_ref=ref, dst_ref=ref, send_sem=send, recv_sem=recv_sem, device_id=(sibling,), device_id_type=MESH
        )

    all_tiles = [stand_in(dgw.at[: BLOCKS - 1, :UNITS], ds_send.at[i], ds_recv.at[i]) for i in range(3)]

    def to_sibling(src, dst, send, recv_sem):
        return pltpu.make_async_remote_copy(
            src_ref=src, dst_ref=dst, send_sem=send, recv_sem=recv_sem, device_id=(sibling,), device_id_type=MESH
        )

    expert_copies = [
        to_sibling(src, dst, ws_send.at[i], ws_recv.at[i])
        for i, (src, dst) in enumerate(
            ((exp_gate, ew.at[:, gate_cols]), (exp_up, ew.at[:, up_cols]), (exp_down, dn.at[down_rows]))
        )
    ]
    tile_forwards = [
        to_sibling(ref, ref, df_send.at[i], df_recv.at[i])
        for i, ref in enumerate((dgw.at[:, tile_rows], duw.at[:, tile_rows], dn.at[tile_down_rows]))
    ]
    for j in range(1, BLOCKS):
        for copy in tile_copies(j):
            copy.start()
    for copy in expert_copies:
        copy.start()

    for copy in small[2:]:
        copy.wait()
    scale = half ** (-0.5)
    lane = lax.broadcasted_iota(jnp.int32, (HEADS, HEAD_DIM), 1)
    head_row = lax.broadcasted_iota(jnp.int32, (HEADS, HEAD_DIM), 0)
    col = lax.broadcasted_iota(jnp.int32, (2 * HEADS, span), 1)
    row = lax.broadcasted_iota(jnp.int32, (2 * HEADS, span), 0)
    own_group = (col % KV_HEADS) == ((row % HEADS) // heads_of)
    head_col = lax.broadcasted_iota(jnp.int32, (HEADS, 1), 0)
    lam_col = jnp.zeros((HEADS, 1), F32)
    for h in range(HEADS):
        lam_col = jnp.where(head_col == h, lam[h], lam_col)
    for copy in key_copies:
        copy.wait()
    scores, owns, vowns = [], [], []
    for s in range(rows):
        q = qscr[s]
        both = jnp.concatenate([jnp.where(lane < half, q, 0.0), jnp.where(lane >= half, q, 0.0)], axis=0)
        kown = jnp.zeros((HEADS, HEAD_DIM), F32)
        vown = jnp.zeros((HEADS, HEAD_DIM), F32)
        for g in range(KV_HEADS):
            mine = head_row // heads_of == g
            part = slice(g * HEAD_DIM, (g + 1) * HEAD_DIM)
            kown = jnp.where(mine, knew[s : s + 1, part], kown)
            vown = jnp.where(mine, vnew[s : s + 1, part], vown)
        owns.append(jnp.sum(both * jnp.concatenate([kown, kown], axis=0), axis=-1, keepdims=True) * scale)
        vowns.append(vown)
        scores.append(
            lax.dot_general(both.astype(BF16), kbuf[s], (((1,), (1,)), ((), ())), preferred_element_type=F32)
        )
    weights, own_weights = [], []
    for s in range(rows):
        valid = own_group & (col < KV_HEADS * lengths[s])
        scaled = jnp.where(valid, scores[s] * scale, -jnp.inf)
        largest = jnp.maximum(jnp.max(scaled, axis=-1, keepdims=True), owns[s])
        raised = jnp.exp(scaled - largest)
        own_raised = jnp.exp(owns[s] - largest)
        inverse = 1.0 / (jnp.sum(raised, axis=-1, keepdims=True) + own_raised)
        prob = raised * inverse
        own_prob = own_raised * inverse
        weights.append((prob[:HEADS] - lam_col * prob[HEADS:]).astype(BF16))
        own_weights.append((own_prob[:HEADS] - lam_col * own_prob[HEADS:]).astype(BF16).astype(F32))
    for copy in value_copies:
        copy.wait()
    for s in range(rows):
        mixed = jnp.dot(weights[s], vbuf[s], preferred_element_type=F32) + own_weights[s] * vowns[s]
        normal = mixed * lax.rsqrt(jnp.mean(mixed * mixed, axis=-1, keepdims=True) + 1e-05)
        normal = normal * head_gain[...]
        for h in range(HEADS):
            hscr[s : s + 1, h * HEAD_DIM : (h + 1) * HEAD_DIM] = normal[h : h + 1, :]
    out_copy.wait()
    state = x + jnp.dot(hscr[...].astype(BF16), obuf[...], preferred_element_type=F32)
    hidden[...] = state
    ffn = state * lax.rsqrt(jnp.mean(state * state, axis=-1, keepdims=True) + 1e-06)
    ffn = (ffn * ffn_gain[...]).astype(BF16)
    ext[:, :width] = ffn
    pieces = jnp.zeros((rows, SIDE), F32)
    branch = branch_gate[...].astype(F32)
    for c in range(width // SIDE):
        pieces += ffn[:, c * SIDE : (c + 1) * SIDE].astype(F32) * branch[c : c + 1, :]
    logit = jnp.sum(pieces, axis=-1, keepdims=True)
    gate = 1.0 / (1.0 + jnp.exp(-logit))
    spot = lax.broadcasted_iota(jnp.int32, (rows, SIDE), 1)
    name = spot % (SIDE // 2)
    table = jnp.where(name == EXPERTS, gate, 0.0)
    token_row = lax.broadcasted_iota(jnp.int32, (rows, SIDE), 0)
    for k in range(routes.shape[0]):
        for s in range(rows):
            here = (name == routes[k, s]) & (name < EXPERTS) & (token_row == s)
            table = table + jnp.where(here, route_weights[k, s], 0.0)
    high = table.astype(BF16).astype(F32)
    ext[:, width:] = jnp.where(spot < SIDE // 2, high, table - high).astype(BF16)

    def spots(c):
        return [place[name] for name in COLOURS[c]]

    def plane_send(c, dp, dq):
        a, p, q = spots(c)
        first, last = IN_COLS[c]
        return pltpu.make_async_remote_copy(
            src_ref=ext.at[:, first:last],
            dst_ref=recv[c].at[(a * T + p) * T + q],
            send_sem=aga_send.at[c],
            recv_sem=aga_recv.at[c * T + dp],
            device_id=(mate(c, 0, dp, dq),),
            device_id_type=MESH,
        )

    def axis_send(c, da, dp):
        a, p, q = spots(c)
        from_p = lax.rem(p + T - dp, T)
        piece = recv[c].at[pl.ds((a * T + from_p) * T, T)]
        return pltpu.make_async_remote_copy(
            src_ref=piece,
            dst_ref=piece,
            send_sem=agb_send.at[c],
            recv_sem=agb_recv.at[c],
            device_id=(mate(c, da, 0, 0),),
            device_id_type=MESH,
        )

    for dp in (2, 1, 3, 0):
        for dq in (2, 1, 3, 0):
            if (dp, dq) != (0, 0):
                for c in range(3):
                    plane_send(c, dp, dq).start()
    for c in range(3):
        a, p, q = spots(c)
        first, last = IN_COLS[c]
        recv[c][(a * T + p) * T + q] = ext[:, first:last]
    for dp in (0, 1, 3, 2):
        for c in range(3):
            ref = recv[c].at[: T - 1 if dp == 0 else T]
            stand_in(ref, aga_send.at[c], aga_recv.at[c * T + dp]).wait_recv()
            for da in (2, 1, 3):
                axis_send(c, da, dp).start()
    for copy in own_loads[:3]:
        copy.wait()
    for copy in all_tiles:
        copy.wait_recv()
    for copy in tile_forwards:
        copy.start()

    def widen(z, y):
        group = z * T + y
        at = pl.ds(pl.multiple_of(group * 16, 16), 16)

        def four(ref, spots_of, cols):
            return jnp.concatenate([ref[i, :, cols].astype(F32) for i in spots_of], axis=0)

        one = four(recv0, [group * T + i for i in range(T)], slice(None))
        xall[at, IN_COLS[0][0] : IN_COLS[0][1]] = one.astype(BF16)
        one = four(recv1, [(i * T + y) * T + z for i in range(T)], slice(None))
        xall[at, IN_COLS[1][0] : IN_COLS[1][1]] = one.astype(BF16)
        where = [(y * T + z) * T + i for i in range(T)]
        one = four(recv2, where, slice(0, width - IN_COLS[2][0]))
        xall[at, IN_COLS[2][0] : width] = one.astype(BF16)
        side[at, :] = four(recv2, where, slice(width - IN_COLS[2][0], None))

    for c in range(3):
        stand_in(recv[c].at[: (T - 1) * T * T], agb_send.at[c], agb_recv.at[c]).wait_recv()
    loop(0, T * T, lambda i: widen(i // T, lax.rem(i, T)))

    for copy in own_loads[3:]:
        copy.wait()
    for copy in expert_copies:
        copy.wait_recv()

    spot = lax.broadcasted_iota(jnp.int32, side.shape, 1) % (SIDE // 2)
    table = side[...]
    routed = jnp.sum(jnp.where(spot == expert, table, 0.0), axis=-1, keepdims=True)
    gate = jnp.sum(jnp.where(spot == EXPERTS, table, 0.0), axis=-1, keepdims=True)
    hid = 2 * ffn_cols
    for n in range(hid // 256):
        cols = slice(n * 256, (n + 1) * 256)
        g = jnp.dot(xall[...], ew[:, cols], preferred_element_type=F32)
        u = jnp.dot(xall[...], ew[:, hid + n * 256 : hid + (n + 1) * 256], preferred_element_type=F32)
        act[:, cols] = (silu(g) * u * routed).astype(BF16)
    for copy in tile_forwards:
        copy.wait_recv()
    across = (((1,), (1,)), ((), ()))
    g = jnp.zeros((all_rows, 2 * UNITS), F32)
    u = jnp.zeros((all_rows, 2 * UNITS), F32)
    for b in range(BLOCKS):
        left = xall[:, b * block_cols : (b + 1) * block_cols]
        g += lax.dot_general(left, dgw[b], across, preferred_element_type=F32)
        u += lax.dot_general(left, duw[b], across, preferred_element_type=F32)
    unit = lax.broadcasted_iota(jnp.int32, g.shape, 1)
    unit = jnp.where(unit >= UNITS, unit - UNITS, unit)
    taken = UNITS - GROUP * (1 - lax.rem(block, 2))
    dact = jnp.where(unit < taken, silu(g) * u * gate, 0.0)
    act[:, hid : hid + 2 * UNITS] = dact.astype(BF16)
    act_perm[...] = jnp.dot(perm[...], act[...], preferred_element_type=F32).astype(BF16)

    def slab(c, a, p):
        return p * T + a if c == 2 else a * T + p

    def axis_sum(c, da, k):
        a, p, q = spots(c)
        return pltpu.make_async_remote_copy(
            src_ref=sendb[c].at[slab(c, lax.rem(a + da, T), lax.rem(p + k, T))],
            dst_ref=recvb[c].at[k * (T - 1) + da - 1],
            send_sem=rsb_send.at[c],
            recv_sem=rsb_recv.at[c * T + k],
            device_id=(mate(c, da, 0, 0),),
            device_id_type=MESH,
        )

    def plane_sum(c, k, l):
        a, p, q = spots(c)
        return pltpu.make_async_remote_copy(
            src_ref=senda[c].at[lax.rem(p + k, T) * T + lax.rem(q + l, T)],
            dst_ref=recva[c].at[k * T + l - 1],
            send_sem=rsa_send.at[c],
            recv_sem=rsa_recv.at[c],
            device_id=(mate(c, 0, k, l),),
            device_id_type=MESH,
        )

    for c in range(3):
        first, last = OUT_COLS[c]
        left = act_perm if c == 1 else act
        part = jnp.dot(left[...], dn[:, first:last], preferred_element_type=F32)
        for i in range(T * T):
            sendb[c][i] = part[i * 16 : (i + 1) * 16].astype(BF16)
        for k in (2, 1, 3, 0):
            for da in (2, 1, 3):
                axis_sum(c, da, k).start()

    for c in range(3):
        stand_in(recv[c].at[: T * T - 1], aga_send.at[c], aga_recv.at[c * T]).wait_send()
        stand_in(recv[c].at[: (T - 1) * T * T], agb_send.at[c], agb_recv.at[c]).wait_send()
    for copy in all_tiles:
        copy.wait_send()
    for copy in expert_copies:
        copy.wait_send()
    for copy in tile_forwards:
        copy.wait_send()

    for k in (2, 1, 3, 0):
        for c in range(3):
            a, p, q = spots(c)
            stand_in(recvb[c].at[: T - 1], rsb_send.at[c], rsb_recv.at[c * T + k]).wait_recv()
            acc = sendb[c][slab(c, a, lax.rem(p + k, T))].astype(F32)
            for i in range(T - 1):
                acc = acc + recvb[c][k * (T - 1) + i].astype(F32)
            for i in range(T):
                senda[c][lax.rem(p + k, T) * T + i] = acc[i * rows : (i + 1) * rows].astype(BF16)
            for l in (2, 1, 3, 0):
                if (k, l) != (0, 0):
                    plane_sum(c, k, l).start()
    for c in range(3):
        stand_in(sendb[c].at[: (T - 1) * T], rsb_send.at[c], rsb_recv.at[c * T]).wait_send()
    for c in range(3):
        a, p, q = spots(c)
        first, last = OUT_COLS[c]
        acc = hidden[:, first:last] + senda[c][p * T + q].astype(F32)
        stand_in(recva[c].at[: T * T - 1], rsa_send.at[c], rsa_recv.at[c]).wait_recv()
        for i in range(T * T - 1):
            acc = acc + recva[c][i].astype(F32)
        out[:, first:last] = acc.astype(BF16)
    for c in range(3):
        stand_in(senda[c].at[: T * T - 1], rsa_send.at[c], rsa_recv.at[c]).wait_send()


def finish_kernel(count, *refs):
    sources, targets, held = refs[:count], refs[count : 2 * count], refs[2 * count : 3 * count]
    in_sem, out_sem = refs[3 * count :]
    ins = [pltpu.make_async_copy(sources[i], held[i], in_sem.at[i]) for i in range(count)]
    outs = [pltpu.make_async_copy(held[i], targets[i], out_sem.at[i]) for i in range(count)]
    for copy in ins:
        copy.start()
    for i in range(count):
        ins[i].wait()
        outs[i].start()
    for copy in outs:
        copy.wait()


def per_device(
    tokens,
    lengths,
    cache_keys,
    cache_values,
    query_w,
    key_w,
    value_w,
    out_w,
    mix_lambda,
    head_gain,
    attn_gain,
    ffn_gain,
    routes,
    route_weights,
    exp_gate,
    exp_up,
    exp_down,
    dense_gate,
    dense_up,
    dense_down,
    branch_gate,
):
    rows, width = tokens.shape
    span = cache_keys.shape[1] * KV_HEADS
    vmem = pl.BlockSpec(memory_space=pltpu.VMEM)
    anywhere = pl.BlockSpec(memory_space=pl.ANY)
    chips = T * T * T
    all_rows = chips * rows
    hid = 2 * exp_gate.shape[1]
    padded = -(-(hid + 2 * UNITS) // 128) * 128
    block_cols = width // BLOCKS
    sem = pltpu.SemaphoreType.DMA
    dense_gate = jnp.swapaxes(dense_gate, 1, 2)
    dense_up = jnp.swapaxes(dense_up, 1, 2)
    routes = routes.T
    route_weights = route_weights.T
    in_cols = [last - first for first, last in IN_COLS]
    out_cols = [last - first for first, last in OUT_COLS]
    results = pl.pallas_call(
        layer_kernel,
        name="layer",
        out_shape=(
            jax.ShapeDtypeStruct((rows, width), BF16),
            jax.ShapeDtypeStruct((rows, key_w.shape[1]), BF16),
            jax.ShapeDtypeStruct((rows, value_w.shape[1]), BF16),
        ),
        in_specs=[anywhere] * 21,
        out_specs=(vmem,) * 3,
        scratch_shapes=[
            pltpu.VMEM((rows, width), BF16),
            pltpu.SMEM(lengths.shape, jnp.int32),
            pltpu.SMEM(mix_lambda.shape, F32),
            pltpu.VMEM((1, HEAD_DIM), F32),
            pltpu.VMEM((1, width), F32),
            pltpu.VMEM((1, width), F32),
            pltpu.SMEM(routes.shape, jnp.int32),
            pltpu.SMEM(route_weights.shape, F32),
            pltpu.VMEM((width // SIDE, SIDE), BF16),
            sem((9,)),
            pltpu.VMEM((rows, width + SIDE), BF16),
            pltpu.VMEM((rows, width), F32),
            pltpu.VMEM((rows, span, HEAD_DIM), BF16),
            pltpu.VMEM((rows, span, HEAD_DIM), BF16),
            pltpu.VMEM(query_w.shape, BF16),
            pltpu.VMEM(key_w.shape, BF16),
            pltpu.VMEM(value_w.shape, BF16),
            pltpu.VMEM(out_w.shape, BF16),
            pltpu.VMEM((rows, HEADS, HEAD_DIM), F32),
            pltpu.VMEM((rows, HEADS * HEAD_DIM), F32),
            sem((3 * QKV_CHUNKS,)),
            sem((rows,)),
            sem((rows,)),
            sem((1,)),
            pltpu.VMEM((width, 2 * hid), BF16),
            pltpu.VMEM((padded, width), BF16),
            pltpu.VMEM((BLOCKS, 2 * UNITS, block_cols), BF16),
            pltpu.VMEM((BLOCKS, 2 * UNITS, block_cols), BF16),
            sem((6,)),
            sem((3,)),
            sem((3,)),
            sem((3,)),
            sem((3,)),
            sem((3,)),
            sem((3,)),
        ]
        + [pltpu.VMEM((chips, rows, cols), BF16) for cols in in_cols]
        + [
            pltpu.VMEM((all_rows, SIDE), F32),
            pltpu.VMEM((all_rows, width), BF16),
            pltpu.VMEM((all_rows, padded), BF16),
            pltpu.VMEM((all_rows, padded), BF16),
            pltpu.VMEM((all_rows, all_rows), BF16),
        ]
        + [pltpu.VMEM((T * T, T * rows, cols), BF16) for cols in out_cols]
        + [pltpu.VMEM(((T - 1) * T, T * rows, cols), BF16) for cols in out_cols]
        + [pltpu.VMEM((T * T, rows, cols), BF16) for cols in out_cols]
        + [pltpu.VMEM((T * T - 1, rows, cols), BF16) for cols in out_cols]
        + [
            sem((3,)),
            sem((3 * T,)),
            sem((3,)),
            sem((3,)),
            sem((3,)),
            sem((3 * T,)),
            sem((3,)),
            sem((3,)),
        ],
        compiler_params=pltpu.CompilerParams(
            collective_id=0, has_side_effects=True, vmem_limit_bytes=63 * 2**20
        ),
    )(
        tokens,
        lengths,
        mix_lambda,
        head_gain.reshape(1, HEAD_DIM),
        attn_gain.reshape(1, width),
        ffn_gain.reshape(1, width),
        routes,
        route_weights,
        branch_gate.reshape(width // SIDE, SIDE),
        cache_keys.reshape(rows, span, HEAD_DIM),
        cache_values.reshape(rows, span, HEAD_DIM),
        query_w,
        key_w,
        value_w,
        out_w,
        exp_gate,
        exp_up,
        exp_down,
        dense_gate,
        dense_up,
        dense_down,
    )
    count = len(results)
    return pl.pallas_call(
        functools.partial(finish_kernel, count),
        name="finish",
        out_shape=tuple(jax.ShapeDtypeStruct(r.shape, r.dtype) for r in results),
        in_specs=[anywhere] * count,
        out_specs=(anywhere,) * count,
        scratch_shapes=[pltpu.VMEM(r.shape, r.dtype) for r in results] + [sem((count,)), sem((count,))],
        compiler_params=pltpu.CompilerParams(vmem_limit_bytes=63 * 2**20),
    )(*results)


def solution(mesh):
    placed = (
        P("ep", None),
        P("ep"),
        P("ep", None, None, None),
        P("ep", None, None, None),
        P(),
        P(),
        P(),
        P(),
        P(),
        P(),
        P(),
        P(),
        P("ep", None),
        P("ep", None),
        P(None, "ep"),
        P(None, "ep"),
        P("ep", None),
        P("ep", None, None),
        P("ep", None, None),
        P("ep", None, None),
        P(),
    )
    return jax.shard_map(
        per_device,
        mesh=mesh,
        in_specs=placed,
        out_specs=(P("ep", None), P("ep", None), P("ep", None)),
        check_vma=False,
    )
```
